32 devices in a mesh: gr: 2 (over x), fs: 4 (over z), tp: 4 (over y, core).
Axes of the slice: x: 2, y: 2, z: 4, core: 2. Of those that a mesh axis runs over, the one named last changes fastest.
Arguments:
- prompt: bfloat16 [4096, 2048], P(('gr', 'fs', 'tp')), may hold values from -6 to 6
- train_gate: float32 [16, 2048, 256], P(None, ('gr', 'fs'), 'tp'), may hold values from -0.125 to 0.125
- train_up: float32 [16, 2048, 256], P(None, ('gr', 'fs'), 'tp'), may hold values from -0.125 to 0.125
- train_down: float32 [16, 256, 2048], P(None, 'tp', ('gr', 'fs')), may hold values from -0.375 to 0.375
- train_shared_gate: float32 [2048, 256], P(('gr', 'fs'), 'tp'), may hold values from -0.125 to 0.125
- train_shared_up: float32 [2048, 256], P(('gr', 'fs'), 'tp'), may hold values from -0.125 to 0.125
- train_shared_down: float32 [256, 2048], P('tp', ('gr', 'fs')), may hold values from -0.375 to 0.375
- norm_gain: float32 [2048], P(('gr', 'fs')), may hold values from 0.1 to 1.9
- expert_ids: int32 [4096, 8], P(('gr', 'fs', 'tp')), may hold values from 0 to 15, all different within a row; in each aligned block of 128 rows (0 to 127, 128 to 255, ...) at most 65 rows name the same one
- route_weight: float32 [4096, 8], P(('gr', 'fs', 'tp')), may hold values from 0.05 to 0.6
Outputs:
- serve_gate: bfloat16 [16, 2048, 256], P(('fs', 'tp'))
- serve_up: bfloat16 [16, 2048, 256], P(('fs', 'tp'))
- serve_down: bfloat16 [16, 256, 2048], P(('fs', 'tp'))
- serve_shared_gate: bfloat16 [2048, 256], P(None, 'tp')
- serve_shared_up: bfloat16 [2048, 256], P(None, 'tp')
- serve_shared_down: bfloat16 [256, 2048], P('tp')
- mixed_out: bfloat16 [4096, 2048], P(('gr', 'fs', 'tp'))
The draws below stay inside these ranges and needn't reach their ends.
Inputs may be any that keep to these rules, and one draw needn't show every extreme that they name: `expert_ids`: each row names 8 different experts. Among the rows of one device no expert is named by more than 65 rows, and in some device's rows one expert is named by exactly 65.
All inputs are finite; a program needn't handle non-finite values.
Results may differ from the reference program's by a relative error of at most 0.012.
Values may be sent and summed in bfloat16 or wider, within the bound.
A program may use at most 128 MiB of HBM per device.

```python
import math
import jax
import jax.numpy as jnp
import numpy as np
from jax import lax

D = 2048
F = 256
SHARED = 256
TOP = 8
TOK_DEV = 128
EXPERTS = 16
SHARED_BLK = 64
CAP = 65
TOKENS = 4096
N_TP = 4


def steps_of(own_key, shape, shards, least, top_value):
    level, own = 1.0, jax.random.fold_in(own_key, 6)
    for position, shards_of in shards:
        heights = jnp.exp(jax.random.uniform(jax.random.fold_in(own, position), (shards_of,), jnp.float32, least / len(shards), top_value / len(shards)))
        level = level * jnp.repeat(heights, shape[position] // shards_of).reshape([-1 if axis == position else 1 for axis in range(len(shape))])
    return level


def shared_out(rng, own, number, rows, count, top, reach, lean):
    sequence = jax.random.permutation(rng, count)
    heavy_load, ordinary = load_shares(count, rows * top, reach, lean, True), load_shares(count, rows * top, reach, lean, False)
    places = jnp.arange(count)

    def named(sizes, turn):
        used = int((sizes > 0).sum())
        fixed = max(1, used // 4)
        shifted = fixed + (places - fixed + turn * (used - fixed)) % max(1, count - fixed)
        return jnp.zeros((count,), jnp.int32).at[sequence[jnp.where(places < fixed, places, shifted)]].set(jnp.asarray(sizes, jnp.int32))

    sizes = jnp.where(number % 4 == 0, named(heavy_load, number // 4), named(ordinary, number - number // 4 - 1))
    mixed = jax.random.permutation(jax.random.fold_in(own, 3), count)
    source_of, receiver = mixed[0:count // 2 * 2:2], mixed[1:count // 2 * 2:2]
    margin = jnp.minimum(sizes[source_of] - 1, reach - sizes[receiver]) // 2
    margin = jnp.where((source_of == sequence[0]) | (receiver == sequence[0]) | (sizes[receiver] == 0), 0, jnp.maximum(margin, 0))
    shifted = jax.random.randint(jax.random.fold_in(own, 4), (count // 2,), 0, 1 << 20) % (margin + 1)
    sizes = sizes.at[source_of].add(-shifted).at[receiver].add(shifted)
    items = jnp.searchsorted(jnp.cumsum(sizes), jnp.arange(rows * top), side="right").astype(jnp.int32)
    table = items.reshape(top, rows).T
    table = table[jax.random.permutation(jax.random.fold_in(own, 1), rows)]
    turn = jax.random.randint(jax.random.fold_in(own, 2), (rows, 1), 0, top)
    return jnp.take_along_axis(table, (jnp.arange(top)[None, :] + turn) % top, axis=1)


def load_shares(count, total, reach, skew, full):
    portions = [(1 << 20) // math.isqrt(rank ** skew) + 1 for rank in range(1, count + 1)]
    largest = reach if full else min(reach, max(-(-total // count), total * portions[0] // sum(portions)))
    least = 1 if total - largest >= count - 1 else 0
    given, rest = [largest] + [least] * (count - 1), total - largest - least * (count - 1)
    while rest > 0:
        free = [i for i in range(1, count) if given[i] < largest] or [i for i in range(1, count) if given[i] < reach]
        pool, remaining = sum([portions[i] for i in free]), rest
        for i in free:
            more = min(reach - given[i], max(1, remaining * portions[i] // pool), rest)
            given[i] = given[i] + more
            rest = rest - more
    return np.array(given)


def bell_draw(key, extent, deviation, reach, shards=(), kind=jnp.bfloat16):
    loudness = steps_of(key, extent, shards, -0.22, 0.18) if shards else 1.0
    array = jax.random.normal(key, extent, jnp.float32) * deviation * loudness
    return jnp.minimum(jnp.maximum(array, -reach), reach).astype(kind)


def setup_inputs(seed: int = 0) -> dict:
    keys = jax.random.split(jax.random.key(seed), 11)
    prompt = bell_draw(keys[0], (TOKENS, D), 1.0, 6.0, ((0, 32),))
    train_gate = bell_draw(keys[1], (EXPERTS, D, F), D ** -0.5, 0.125, ((1, 8), (2, 4)), jnp.float32)
    train_up = bell_draw(keys[2], (EXPERTS, D, F), D ** -0.5, 0.125, ((1, 8), (2, 4)), jnp.float32)
    train_down = bell_draw(keys[3], (EXPERTS, F, D), F ** -0.5, 0.375, ((1, 4), (2, 8)), jnp.float32)
    train_shared_gate = bell_draw(keys[4], (D, SHARED), D ** -0.5, 0.125, ((0, 8), (1, 4)), jnp.float32)
    train_shared_up = bell_draw(keys[5], (D, SHARED), D ** -0.5, 0.125, ((0, 8), (1, 4)), jnp.float32)
    train_shared_down = bell_draw(keys[6], (SHARED, D), SHARED ** -0.5, 0.375, ((0, 4), (1, 8)), jnp.float32)
    norm_gain = jnp.clip(1.0 + 0.18 * jax.random.normal(keys[7], (D,), jnp.float32), 0.1, 1.9)
    expert_ids_keys = jax.random.split(jax.random.fold_in(keys[8], 1), TOKENS // TOK_DEV)
    expert_ids_turns = jax.random.permutation(jax.random.fold_in(keys[8], 3), TOKENS // TOK_DEV)
    expert_ids = jax.vmap(lambda own, number: shared_out(jax.random.fold_in(keys[8], 2), own, number, TOK_DEV, EXPERTS, TOP, CAP, 1))(expert_ids_keys, expert_ids_turns).reshape((TOKENS, TOP))
    route_weight = jnp.clip(0.05 + 0.55 * jax.random.uniform(keys[9], (TOKENS, TOP), jnp.float32) ** steps_of(keys[9], (TOKENS, TOP), ((0, 32),), -0.2, 0.2), 0.05, 0.6)
    return {"prompt": prompt, "train_gate": train_gate, "train_up": train_up, "train_down": train_down, "train_shared_gate": train_shared_gate, "train_shared_up": train_shared_up, "train_shared_down": train_shared_down, "norm_gain": norm_gain, "expert_ids": expert_ids, "route_weight": route_weight}


eps_norm = 1e-06

def swiglu_rows(inputs, gate_w, up_w, down_w):
    gate_val = jnp.dot(inputs, gate_w, preferred_element_type=jnp.float32)
    up_val = jnp.dot(inputs, up_w, preferred_element_type=jnp.float32)
    hidden = (jax.nn.silu(gate_val) * up_val).astype(jnp.bfloat16)
    return jnp.dot(hidden, down_w, preferred_element_type=jnp.float32).astype(jnp.bfloat16)

def reference(prompt, train_gate, train_up, train_down, train_shared_gate, train_shared_up, train_shared_down, norm_gain, expert_ids, route_weight):
    gain_col = norm_gain[:, None]
    serve_gate = (train_gate * gain_col[None]).astype(jnp.bfloat16)
    serve_up = (train_up * gain_col[None]).astype(jnp.bfloat16)
    serve_down = train_down.astype(jnp.bfloat16)
    serve_shared_gate = (train_shared_gate * gain_col).astype(jnp.bfloat16)
    serve_shared_up = (train_shared_up * gain_col).astype(jnp.bfloat16)
    serve_shared_down = train_shared_down.astype(jnp.bfloat16)
    widened = prompt.astype(jnp.float32)
    normed = (widened * lax.rsqrt(lax.optimization_barrier(jnp.mean(widened * widened, axis=-1, keepdims=True)) + eps_norm)).astype(jnp.bfloat16)
    shared_act = (jax.nn.silu(jnp.dot(normed, serve_shared_gate, preferred_element_type=jnp.float32)) * jnp.dot(normed, serve_shared_up, preferred_element_type=jnp.float32)).astype(jnp.bfloat16)
    shared_sum = jnp.zeros((TOKENS, D), jnp.float32)
    for column in range(N_TP):
        first_row = column * SHARED_BLK
        partial_out = jnp.dot(shared_act[:, first_row:first_row + SHARED_BLK], serve_shared_down[first_row:first_row + SHARED_BLK], preferred_element_type=jnp.float32).astype(jnp.bfloat16)
        partial_out = lax.optimization_barrier(partial_out)
        shared_sum = shared_sum + partial_out.astype(jnp.float32)
    blocks = TOKENS // TOK_DEV
    flat_ids = expert_ids.reshape(blocks, TOK_DEV * TOP).astype(jnp.int32)
    onehot = (flat_ids[:, :, None] == jnp.arange(EXPERTS, dtype=jnp.int32)[None, None, :]).astype(jnp.int32)
    earlier = jnp.cumsum(onehot, axis=1) - onehot
    places = lax.optimization_barrier(jnp.sum(earlier * onehot, axis=-1)).astype(jnp.int32)
    block_ids = jnp.arange(blocks, dtype=jnp.int32)[:, None]
    token_ids = block_ids * TOK_DEV + jnp.arange(TOK_DEV * TOP, dtype=jnp.int32)[None, :] // TOP
    target = ((flat_ids * blocks + block_ids) * CAP + places).reshape(-1).astype(jnp.int32)
    row_table = jnp.full((EXPERTS * blocks * CAP,), TOKENS, jnp.int32).at[target].set(token_ids.reshape(-1).astype(jnp.int32)).reshape(EXPERTS, blocks * CAP)
    row_weights = jnp.zeros((EXPERTS * blocks * CAP,), jnp.float32).at[target].set(route_weight.reshape(-1)).reshape(EXPERTS, blocks * CAP)
    padded_rows = jnp.concatenate([normed, jnp.zeros((1, D), jnp.bfloat16)], axis=0)

    def add_expert(totals, expert_data):
        rows_index, weights_here, gate_w, up_w, down_w = expert_data
        outputs = swiglu_rows(padded_rows[rows_index], gate_w, up_w, down_w)
        return (totals.at[rows_index].add(weights_here[:, None] * outputs.astype(jnp.float32)), None)
    totals, _ = lax.scan(add_expert, jnp.zeros((TOKENS + 1, D), jnp.float32), (row_table, row_weights, serve_gate, serve_up, serve_down))
    mixed_out = (totals[:TOKENS] + shared_sum).astype(jnp.bfloat16)
    return (serve_gate, serve_up, serve_down, serve_shared_gate, serve_shared_up, serve_shared_down, mixed_out)
```

```python
import functools

import jax
import jax.numpy as jnp
from jax import lax
from jax.experimental import pallas as pl
from jax.experimental.pallas import tpu as pltpu
from jax.sharding import PartitionSpec as P

eps_norm = 1e-06
MESH = pl.DeviceIdType.MESH
CORES = 2
VMEM_PLAN = 40 * 2**20
VMEM_LIMIT = 60 * 2**20


def gather_kernel(
    n_gr, n_fs, n_tp,
    x_in, w_in, gu_in, dn_in, sgu_in, sdn_in,
    x_out, w_out, gu_out, dn_out, sgu_out, sdn_out,
    xr, wr, gr_sem, dr_sem, sgr, sdr, zs, ys, cs, as_, fs_sem, ss, loc,
):
    gr, z, tp = lax.axis_index("gr"), lax.axis_index("fs"), lax.axis_index("tp")
    y, c = tp // CORES, tp % CORES
    y_peer = (1 - y) * CORES + c
    c_peer = y * CORES + 1 - c
    x_peer = 1 - gr
    rows_d = sgu_in.shape[0]
    cols_d = sdn_in.shape[1]
    hid = sdn_in.shape[0]

    barrier = pltpu.get_barrier_semaphore()
    for dz in range(n_fs):
        for dt in range(n_tp):
            if dz == 0 and dt == 0:
                continue
            pl.semaphore_signal(
                barrier, inc=1, device_id_type=MESH,
                device_id={"gr": gr, "fs": (z + dz) % n_fs, "tp": (tp + dt) % n_tp},
            )
    pl.semaphore_signal(
        barrier, inc=1, device_id={"gr": x_peer, "fs": z, "tp": tp}, device_id_type=MESH
    )
    pl.semaphore_wait(barrier, n_fs * n_tp)

    def dev(g, f, t):
        return {"gr": g, "fs": f, "tp": t}

    def remote(src, dst, send, recv, where):
        return pltpu.make_async_remote_copy(
            src_ref=src, dst_ref=dst, send_sem=send, recv_sem=recv,
            device_id=where, device_id_type=MESH,
        )

    def gu_at(g, f, t):
        return gu_out.at[t, pl.ds(pl.multiple_of((g * n_fs + f) * rows_d, 128), rows_d), :]

    def dn_at(g, f, t):
        return dn_out.at[
            pl.ds(pl.multiple_of(t * hid, 16), hid),
            pl.ds(pl.multiple_of((g * n_fs + f) * cols_d, 128), cols_d),
        ]

    def sgu_at(g, f):
        return sgu_out.at[pl.ds(pl.multiple_of((g * n_fs + f) * rows_d, 128), rows_d), :]

    def sdn_at(g, f):
        return sdn_out.at[:, pl.ds(pl.multiple_of((g * n_fs + f) * cols_d, 128), cols_d)]

    def block(src_own, owner, sems, slot, where):
        xs = x_in if src_own else x_out.at[owner]
        ws = w_in if src_own else w_out.at[owner]
        return (
            remote(xs, x_out.at[owner], sems.at[slot, 0], xr.at[owner], where),
            remote(ws, w_out.at[owner], sems.at[slot, 1], wr.at[owner], where),
        )

    def shared(src_own, g, f, sems, slot, where):
        gs = sgu_in if src_own else sgu_at(g, f)
        ds_ = sdn_in if src_own else sdn_at(g, f)
        k = g * n_fs + f
        return (
            remote(gs, sgu_at(g, f), sems.at[slot, 0], sgr.at[k], where),
            remote(ds_, sdn_at(g, f), sems.at[slot, 1], sdr.at[k], where),
        )

    def expert(src_own, f, t, slot):
        gs = gu_in.at[z * n_tp + tp] if src_own else gu_at(gr, f, t)
        ds_ = dn_in.at[z * n_tp + tp] if src_own else dn_at(gr, f, t)
        k = gr * (n_fs * n_tp) + f * n_tp + t
        where = dev(x_peer, z, tp)
        return (
            remote(gs, gu_at(gr, f, t), fs_sem.at[slot, 0], gr_sem.at[k], where),
            remote(ds_, dn_at(gr, f, t), fs_sem.at[slot, 1], dr_sem.at[k], where),
        )

    def start(copies):
        for one in copies:
            one.start()

    own = tp * n_fs + z
    up, down = dev(gr, z + 1, tp), dev(gr, z - 1, tp)
    has_up, has_down = z < n_fs - 1, z > 0
    to_y, to_c, to_x = dev(gr, z, y_peer), dev(gr, z, c_peer), dev(x_peer, z, tp)
    pending = []

    def go(cond, copies):
        pending.append((cond, copies))
        if cond is None:
            start(copies)
        else:
            pl.when(cond)(lambda: start(copies))

    go(None, expert(True, z, tp, 0))
    go(None, shared(True, gr, z, ss, 0, to_x))
    go(has_up, block(True, own, zs, 0, up))
    go(has_down, block(True, own, zs, 1, down))
    go(None, block(True, own, ys, 0, to_y))
    go(None, block(True, own, cs, 0, to_c))
    go(has_up, shared(True, gr, z, ss, 1, up))
    go(has_down, shared(True, gr, z, ss, 2, down))
    locals_ = [
        pltpu.make_async_copy(x_in, x_out.at[own], loc.at[0]),
        pltpu.make_async_copy(w_in, w_out.at[own], loc.at[1]),
        pltpu.make_async_copy(gu_in.at[z * n_tp + tp], gu_at(gr, z, tp), loc.at[2]),
        pltpu.make_async_copy(dn_in.at[z * n_tp + tp], dn_at(gr, z, tp), loc.at[3]),
        pltpu.make_async_copy(sgu_in, sgu_at(gr, z), loc.at[4]),
        pltpu.make_async_copy(sdn_in, sdn_at(gr, z), loc.at[5]),
    ]
    start(locals_)

    a2a = []
    for dz in range(n_fs):
        for dt in range(n_tp):
            if dz == 0 and dt == 0:
                continue
            f, t = (z + dz) % n_fs, (tp + dt) % n_tp
            e, k = f * n_tp + t, dz * n_tp + dt
            mine = gr * (n_fs * n_tp) + z * n_tp + tp
            pair = (
                remote(gu_in.at[e], gu_at(gr, z, tp), as_.at[k, 0], gr_sem.at[mine], dev(gr, f, t)),
                remote(dn_in.at[e], dn_at(gr, z, tp), as_.at[k, 1], dr_sem.at[mine], dev(gr, f, t)),
            )
            start(pair)
            a2a.append(pair)

    def wait_expert(g, f, t):
        k = g * (n_fs * n_tp) + f * n_tp + t
        remote(gu_in.at[0], gu_at(g, f, t), as_.at[0, 0], gr_sem.at[k], to_x).wait_recv()
        remote(dn_in.at[0], dn_at(g, f, t), as_.at[0, 1], dr_sem.at[k], to_x).wait_recv()

    def wait_block(owner):
        for one in block(True, owner, cs, 0, to_c):
            one.wait_recv()

    def wait_shared(g, f):
        for one in shared(True, g, f, ss, 0, to_x):
            one.wait_recv()

    def pass_experts(dz):
        for dt in range(n_tp):
            if dz == 0 and dt == 0:
                continue
            f, t = (z + n_fs - dz) % n_fs, (tp + n_tp - dt) % n_tp
            wait_expert(gr, f, t)
            go(None, expert(False, f, t, dz * n_tp + dt))

    pass_experts(0)
    for d in range(1, n_fs):
        for way in (0, 1):
            f = z - d if way == 0 else z + d
            there = f >= 0 if way == 0 else f < n_fs
            more = has_up if way == 0 else has_down
            onward = up if way == 0 else down
            owner = tp * n_fs + f

            @pl.when(there)
            def _(f=f, owner=owner):
                wait_block(owner)
                wait_shared(gr, f)

            slot = 2 * d + way
            go(there & more, block(False, owner, zs, slot, onward))
            go(there, block(False, owner, ys, slot, to_y))
            go(there & more, shared(False, gr, f, ss, 2 * slot + 1, onward))
            go(there, shared(False, gr, f, ss, 2 * slot, to_x))
            go(there, block(False, owner, cs, slot, to_c))
        pass_experts(d)
    for k in range(n_fs):
        f = (z + k) % n_fs
        owner = y_peer * n_fs + f
        wait_block(owner)
        go(None, block(False, owner, cs, 2 * n_fs + k, to_c))
    for f in range(n_fs):
        for dt in range(n_tp):
            wait_expert(x_peer, f, dt)
        wait_shared(x_peer, f)
        for yy in range(n_tp // CORES):
            wait_block((yy * CORES + 1 - c) * n_fs + f)
    for one in locals_:
        one.wait()
    for pair in a2a:
        for one in pair:
            one.wait_send()
    for cond, copies in pending:
        if cond is None:
            for one in copies:
                one.wait_send()
        else:

            @pl.when(cond)
            def _(copies=copies):
                for one in copies:
                    one.wait_send()


def reduce_kernel(
    n_fs, n_tp,
    x_ref, w_ref, g_ref, u_ref, dn_ref, sgu_ref, sdn_ref,
    out_ref,
    part, rc, ry, ru, rd, sh, cs, cr, ys, yr, us, ur, ds_, dr,
):
    gr, z, tp = lax.axis_index("gr"), lax.axis_index("fs"), lax.axis_index("tp")
    y, c = tp // CORES, tp % CORES
    has_up, has_down = z < n_fs - 1, z > 0
    to_c = {"gr": gr, "fs": z, "tp": y * CORES + 1 - c}
    to_y = {"gr": gr, "fs": z, "tp": (1 - y) * CORES + c}
    up, down = {"gr": gr, "fs": z + 1, "tp": tp}, {"gr": gr, "fs": z - 1, "tp": tp}
    rows, width = x_ref.shape[1], x_ref.shape[2]
    half = sdn_ref.shape[0]

    barrier = pltpu.get_barrier_semaphore()
    pl.semaphore_signal(barrier, inc=1, device_id=to_c, device_id_type=MESH)
    pl.semaphore_signal(barrier, inc=1, device_id=to_y, device_id_type=MESH)

    @pl.when(has_up)
    def _():
        pl.semaphore_signal(barrier, inc=1, device_id=up, device_id_type=MESH)

    @pl.when(has_down)
    def _():
        pl.semaphore_signal(barrier, inc=1, device_id=down, device_id_type=MESH)

    pl.semaphore_wait(barrier, 2 + has_up.astype(jnp.int32) + has_down.astype(jnp.int32))

    def remote(src, dst, send, recv, where):
        return pltpu.make_async_remote_copy(
            src_ref=src, dst_ref=dst, send_sem=send, recv_sem=recv,
            device_id=where, device_id_type=MESH,
        )

    step = 2
    chunk = min(width, 512)

    def compute(group):
        def rows_of(k, carry):
            first = group * n_fs + k * step
            xs = x_ref[pl.ds(first, step)].reshape(step * rows, width)
            ws = w_ref[pl.ds(first, step)].reshape(step * rows, 1)
            gate = jnp.dot(xs, g_ref[...], preferred_element_type=jnp.float32)
            upv = jnp.dot(xs, u_ref[...], preferred_element_type=jnp.float32)
            act = (jax.nn.silu(gate) * upv * ws).astype(jnp.bfloat16)
            sh[...] = jnp.zeros_like(sh)

            @pl.when(z // step == k)
            def _():
                both = jnp.dot(
                    x_ref[group * n_fs + z], sgu_ref[...], preferred_element_type=jnp.float32
                )
                val = jax.nn.silu(both[:, :half]) * both[:, half:]
                sh[pl.ds(pl.multiple_of((z % step) * rows, 128), rows), :] = val.astype(jnp.bfloat16)

            shared = sh[...]

            def cols_of(j, inner):
                cols = pl.ds(pl.multiple_of(j * chunk, 128), chunk)
                res = jnp.dot(act, dn_ref[:, cols], preferred_element_type=jnp.float32)
                res = res + jnp.dot(shared, sdn_ref[:, cols], preferred_element_type=jnp.float32)
                part[pl.ds(first, step), :, cols] = res.astype(jnp.bfloat16).reshape(
                    step, rows, chunk
                )
                return inner

            return lax.fori_loop(0, width // chunk, cols_of, carry)

        lax.fori_loop(0, n_fs // step, rows_of, 0)

    other_y, other_c = 1 - y, 1 - c
    c_sends = []

    def groups(i, carry):
        gy = jnp.where(i % 2 == 0, other_y, y)
        gc = jnp.where(i < 2, other_c, c)
        group = gy * CORES + gc
        compute(group)

        @pl.when(i < 2)
        def _():
            remote(
                part.at[pl.ds(group * n_fs, n_fs)], rc.at[i % 2], cs.at[i % 2], cr.at[i % 2], to_c
            ).start()

        return carry

    lax.fori_loop(0, 4, groups, 0)

    def c_copy(i, gy):
        group = gy * CORES + other_c
        return remote(part.at[pl.ds(group * n_fs, n_fs)], rc.at[i], cs.at[i], cr.at[i], to_c)

    c_copy(0, other_y).wait_recv()
    g_y = other_y * CORES + c
    g_own = tp

    def wide(v):
        return v.astype(jnp.float32)

    spots = []
    for d in range(n_fs - 1, -1, -1):
        for way in (0, 1):
            if d == 0 and way == 1:
                continue
            t = z + d if way == 0 else z - d
            spots.append((d, way, t, (t < n_fs) if way == 0 else (t >= 0)))

    def y_copy(t):
        return remote(part.at[g_y * n_fs + t], ry.at[t], ys.at[t], yr.at[t], to_y)

    for d, way, t, there in spots:

        @pl.when(there)
        def _(t=t):
            part[g_y * n_fs + t] = (wide(part[g_y * n_fs + t]) + wide(rc[0, t])).astype(jnp.bfloat16)
            y_copy(t).start()

    c_copy(1, y).wait_recv()

    def u_copy(t):
        return remote(part.at[g_own * n_fs + t], ru.at[t], us.at[t], ur.at[t], up)

    def d_copy(t):
        return remote(part.at[g_own * n_fs + t], rd.at[t], ds_.at[t], dr.at[t], down)

    for d, way, t, there in spots:

        @pl.when(there)
        def _(d=d, way=way, t=t):
            y_copy(t).wait_recv()
            total = wide(part[g_own * n_fs + t]) + wide(rc[1, t]) + wide(ry[t])
            if d == 0:
                out_ref[...] = total.astype(jnp.bfloat16)

                @pl.when(has_down & has_up)
                def _():
                    u_copy(t).wait_recv()
                    d_copy(t).wait_recv()
                    out_ref[...] = (total + wide(ru[t]) + wide(rd[t])).astype(jnp.bfloat16)

                @pl.when(has_down & jnp.logical_not(has_up))
                def _():
                    u_copy(t).wait_recv()
                    out_ref[...] = (total + wide(ru[t])).astype(jnp.bfloat16)

                @pl.when(has_up & jnp.logical_not(has_down))
                def _():
                    d_copy(t).wait_recv()
                    out_ref[...] = (total + wide(rd[t])).astype(jnp.bfloat16)
            else:
                copy, arrived, before = (
                    (u_copy, ru, has_down) if way == 0 else (d_copy, rd, has_up)
                )
                part[g_own * n_fs + t] = total.astype(jnp.bfloat16)

                @pl.when(before)
                def _():
                    copy(t).wait_recv()
                    part[g_own * n_fs + t] = (total + wide(arrived[t])).astype(jnp.bfloat16)

                copy(t).start()

    c_copy(0, other_y).wait_send()
    c_copy(1, y).wait_send()
    for d, way, t, there in spots:

        @pl.when(there)
        def _(d=d, way=way, t=t):
            y_copy(t).wait_send()
            if d:
                (u_copy if way == 0 else d_copy)(t).wait_send()


def small_body(
    n_gr, n_fs, n_tp,
    prompt, train_gate, train_up, train_down, train_shared_gate, train_shared_up,
    train_shared_down, norm_gain, expert_ids, route_weight,
):
    experts, rows_d, hid = train_gate.shape
    cols_d = train_down.shape[2]
    rows, width = prompt.shape
    plane = n_fs * n_tp
    gain_col = norm_gain[:, None]
    gu = jnp.concatenate(
        (train_gate * gain_col[None], train_up * gain_col[None]), axis=2
    ).astype(jnp.bfloat16)
    dn = train_down.astype(jnp.bfloat16)
    sgu = jnp.concatenate(
        (train_shared_gate * gain_col, train_shared_up * gain_col), axis=1
    ).astype(jnp.bfloat16)
    sdn = train_shared_down.astype(jnp.bfloat16)
    widened = prompt.astype(jnp.float32)
    normed = (
        widened * lax.rsqrt(jnp.mean(widened * widened, axis=-1, keepdims=True) + eps_norm)
    ).astype(jnp.bfloat16)
    named = expert_ids.T[None, :, :] == jnp.arange(experts, dtype=jnp.int32)[:, None, None]
    weights = jnp.sum(jnp.where(named, route_weight.T[None, :, :], 0.0), axis=1)

    bf16 = jnp.bfloat16
    vmem = pl.BlockSpec(memory_space=pltpu.VMEM)
    dma = pltpu.SemaphoreType.DMA
    full = n_gr * n_fs
    rows_all, weights_all, gu_all, serve_down, sgu_all, serve_shared_down = pl.pallas_call(
        functools.partial(gather_kernel, n_gr, n_fs, n_tp),
        out_shape=(
            jax.ShapeDtypeStruct((plane, rows, width), bf16),
            jax.ShapeDtypeStruct((plane, experts, rows), jnp.float32),
            jax.ShapeDtypeStruct((n_tp, full * rows_d, 2 * hid), bf16),
            jax.ShapeDtypeStruct((n_tp * hid, full * cols_d), bf16),
            jax.ShapeDtypeStruct((full * rows_d, 2 * hid), bf16),
            jax.ShapeDtypeStruct((hid, full * cols_d), bf16),
        ),
        in_specs=[vmem] * 6,
        out_specs=(vmem,) * 6,
        scratch_shapes=[
            dma((plane,)), dma((plane,)),
            dma((n_gr * plane,)), dma((n_gr * plane,)),
            dma((full,)), dma((full,)),
            dma((2 * n_fs, 2)), dma((2 * n_fs, 2)), dma((3 * n_fs, 2)),
            dma((plane, 2)), dma((plane, 2)), dma((4 * n_fs, 2)), dma((6,)),
        ],
        compiler_params=pltpu.CompilerParams(
            collective_id=0, has_side_effects=True, vmem_limit_bytes=VMEM_LIMIT
        ),
    )(normed, weights, gu, dn, sgu, sdn)
    serve_gate = jnp.concatenate([gu_all[t, :, :hid] for t in range(n_tp)], axis=1)
    serve_up = jnp.concatenate([gu_all[t, :, hid:] for t in range(n_tp)], axis=1)
    own = lax.axis_index("fs") * n_tp + lax.axis_index("tp")
    own_weights = lax.dynamic_index_in_dim(weights_all, own, axis=1, keepdims=False)[:, :, None]
    mixed_out = pl.pallas_call(
        functools.partial(reduce_kernel, n_fs, n_tp),
        out_shape=jax.ShapeDtypeStruct((rows, width), bf16),
        in_specs=[vmem] * 7,
        out_specs=vmem,
        scratch_shapes=[
            pltpu.VMEM((plane, rows, width), bf16),
            pltpu.VMEM((2, n_fs, rows, width), bf16),
            pltpu.VMEM((n_fs, rows, width), bf16),
            pltpu.VMEM((n_fs, rows, width), bf16),
            pltpu.VMEM((n_fs, rows, width), bf16),
            pltpu.VMEM((2 * rows, hid), bf16),
            dma((2,)), dma((2,)),
            dma((n_fs,)), dma((n_fs,)), dma((n_fs,)), dma((n_fs,)), dma((n_fs,)), dma((n_fs,)),
        ],
        compiler_params=pltpu.CompilerParams(
            collective_id=1, has_side_effects=True, vmem_limit_bytes=VMEM_LIMIT
        ),
    )(rows_all, own_weights, serve_gate, serve_up, serve_down, sgu_all, serve_shared_down)
    return (
        serve_gate[None], serve_up[None], serve_down[None],
        sgu_all[:, :hid], sgu_all[:, hid:], serve_shared_down, mixed_out,
    )


def regroup(stacked, lowered):
    stacked = lax.all_to_all(
        lax.all_to_all(stacked, "fs", split_axis=0, concat_axis=2, tiled=True),
        "tp",
        split_axis=0,
        concat_axis=3,
        tiled=True,
    )
    lowered = lax.all_to_all(
        lax.all_to_all(lowered, "fs", split_axis=0, concat_axis=2, tiled=True),
        "tp",
        split_axis=0,
        concat_axis=1,
        tiled=True,
    )
    return (stacked, lowered)


def body(
    prompt,
    train_gate,
    train_up,
    train_down,
    train_shared_gate,
    train_shared_up,
    train_shared_down,
    norm_gain,
    expert_ids,
    route_weight,
):
    gain_col = norm_gain[:, None]
    stacked = jnp.stack((train_gate * gain_col[None], train_up * gain_col[None]), axis=1).astype(
        jnp.bfloat16
    )
    lowered = train_down.astype(jnp.bfloat16)
    stacked, lowered = regroup(stacked, lowered)
    stacked, lowered = (
        lax.all_gather(stacked, "gr", axis=2, tiled=True),
        lax.all_gather(lowered, "gr", axis=2, tiled=True),
    )
    serve_gate = stacked[:, 0]
    serve_up = stacked[:, 1]
    serve_shared_gate, serve_shared_up, serve_shared_down = (
        lax.all_gather(
            (train_shared_gate * gain_col).astype(jnp.bfloat16), ("gr", "fs"), axis=0, tiled=True
        ),
        lax.all_gather(
            (train_shared_up * gain_col).astype(jnp.bfloat16), ("gr", "fs"), axis=0, tiled=True
        ),
        lax.all_gather(train_shared_down.astype(jnp.bfloat16), ("gr", "fs"), axis=1, tiled=True),
    )
    widened = prompt.astype(jnp.float32)
    normed = (
        widened * lax.rsqrt(jnp.mean(widened * widened, axis=-1, keepdims=True) + eps_norm)
    ).astype(jnp.bfloat16)
    block_rows = lax.all_gather(normed, "tp", axis=0, tiled=True)
    gate_val = jnp.dot(block_rows, serve_shared_gate, preferred_element_type=jnp.float32)
    up_val = jnp.dot(block_rows, serve_shared_up, preferred_element_type=jnp.float32)
    shared_act = (jax.nn.silu(gate_val) * up_val).astype(jnp.bfloat16)
    shared_sum = lax.psum_scatter(
        jnp.dot(shared_act, serve_shared_down, preferred_element_type=jnp.float32).astype(
            jnp.bfloat16
        ),
        "tp",
        scatter_dimension=0,
        tiled=True,
    ).astype(jnp.float32)
    row_count = prompt.shape[0]
    top_count = expert_ids.shape[1]
    model_width = prompt.shape[1]
    expert_count = lax.axis_size("fs") * lax.axis_size("tp")
    capacity = row_count * top_count // expert_count + 1
    flat_ids = expert_ids.reshape(-1)
    onehot = (flat_ids[:, None] == jnp.arange(expert_count, dtype=jnp.int32)[None, :]).astype(
        jnp.int32
    )
    earlier = jnp.cumsum(onehot, axis=0) - onehot
    places = jnp.sum(earlier * onehot, axis=1)
    slot_ids = (flat_ids * capacity + places).reshape(row_count, top_count)
    slot_range = jnp.arange(expert_count * capacity, dtype=jnp.int32)
    dispatch = jnp.any(slot_range[:, None, None] == slot_ids[None, :, :], axis=-1).astype(
        jnp.bfloat16
    )
    outgoing = jnp.dot(dispatch, normed, preferred_element_type=jnp.float32).astype(jnp.bfloat16)
    outgoing = outgoing.reshape(expert_count, capacity, model_width)
    arrived = lax.all_to_all(outgoing, ("fs", "tp"), split_axis=0, concat_axis=0, tiled=True)
    source_count, slot_count, width_here = arrived.shape
    arrived_rows = arrived.reshape(source_count * slot_count, width_here)
    gate_val = jnp.dot(arrived_rows, serve_gate[0], preferred_element_type=jnp.float32)
    up_val = jnp.dot(arrived_rows, serve_up[0], preferred_element_type=jnp.float32)
    hidden = (jax.nn.silu(gate_val) * up_val).astype(jnp.bfloat16)
    result = jnp.dot(hidden, lowered[0], preferred_element_type=jnp.float32).astype(jnp.bfloat16)
    result = result.reshape(source_count, slot_count, width_here)
    returned = lax.all_to_all(result, ("fs", "tp"), split_axis=0, concat_axis=0, tiled=True)
    picked = returned.reshape(expert_count * capacity, model_width)[slot_ids]
    routed = jnp.sum(route_weight[:, :, None] * picked.astype(jnp.float32), axis=1)
    mixed_out = (routed + shared_sum).astype(jnp.bfloat16)
    return (
        serve_gate,
        serve_up,
        lowered,
        serve_shared_gate,
        serve_shared_up,
        serve_shared_down,
        mixed_out,
    )


def solution(mesh):
    placed = (
        P(("gr", "fs", "tp"), None),
        P(None, ("gr", "fs"), "tp"),
        P(None, ("gr", "fs"), "tp"),
        P(None, "tp", ("gr", "fs")),
        P(("gr", "fs"), "tp"),
        P(("gr", "fs"), "tp"),
        P("tp", ("gr", "fs")),
        P(("gr", "fs")),
        P(("gr", "fs", "tp"), None),
        P(("gr", "fs", "tp"), None),
    )
    n_gr, n_fs, n_tp = (mesh.shape[name] for name in ("gr", "fs", "tp"))

    def chosen(prompt, *rest):
        held = n_fs * n_tp * prompt.size * prompt.dtype.itemsize * 5 // 2
        if n_gr == 2 and n_tp == 2 * CORES and n_fs % 2 == 0 and held < VMEM_PLAN:
            return small_body(n_gr, n_fs, n_tp, prompt, *rest)
        return body(prompt, *rest)

    return jax.shard_map(
        chosen,
        mesh=mesh,
        in_specs=placed,
        out_specs=(
            P(("fs", "tp"), None, None),
            P(("fs", "tp"), None, None),
            P(("fs", "tp"), None, None),
            P(None, "tp"),
            P(None, "tp"),
            P("tp", None),
            P(("gr", "fs", "tp"), None),
        ),
        check_vma=False,
    )
```

```python
import functools

import jax
import jax.numpy as jnp
from jax import lax
from jax.experimental import pallas as pl
from jax.experimental.pallas import tpu as pltpu
from jax.sharding import PartitionSpec as P

eps_norm = 1e-06
MESH = pl.DeviceIdType.MESH
CORES = 2
VMEM_PLAN = 40 * 2**20
VMEM_LIMIT = 60 * 2**20


def plane_kernel(
    n_gr, n_fs, n_tp, parts,
    x_in, w_in, e_in, s_in,
    gate_out, up_out, down_out, s_out, mixed_out,
    x_all, w_all, e_all, s_gu, part, rc, ry, ru, rd, sh,
    xr, wr, er, sr, zs, ys, cs, as_, fs_sem, ss, loc,
    ks, kr, qs, qr, us, ur, ds_, dr,
):
    gr, z, tp = lax.axis_index("gr"), lax.axis_index("fs"), lax.axis_index("tp")
    y, c = tp // CORES, tp % CORES
    y_peer = (1 - y) * CORES + c
    c_peer = y * CORES + 1 - c
    x_peer = 1 - gr
    plane = n_fs * n_tp
    _, hid, cols_d = s_in.shape
    sub, width = x_in.shape[1], x_in.shape[2]
    rows = parts * sub

    def dev(g, f, t):
        return {"gr": g, "fs": f, "tp": t}

    peers = [
        (dz, dt, (z + dz) % n_fs, (tp + dt) % n_tp)
        for dz in range(n_fs)
        for dt in range(n_tp)
        if dz or dt
    ]
    barrier = pltpu.get_barrier_semaphore()
    for _, _, f, t in peers:
        pl.semaphore_signal(barrier, inc=1, device_id=dev(gr, f, t), device_id_type=MESH)
    pl.semaphore_signal(barrier, inc=1, device_id=dev(x_peer, z, tp), device_id_type=MESH)
    pl.semaphore_wait(barrier, plane)

    def remote(src, dst, send, recv, where):
        return pltpu.make_async_remote_copy(
            src_ref=src, dst_ref=dst, send_sem=send, recv_sem=recv,
            device_id=where, device_id_type=MESH,
        )

    def cols_of(g, f):
        return pl.ds(pl.multiple_of((g * n_fs + f) * cols_d, 128), cols_d)

    def e_at(g, f, t):
        return e_all.at[:, pl.ds(pl.multiple_of(t * hid, 16), hid), cols_of(g, f)]

    def s_at(g, f):
        return s_out.at[:, :, cols_of(g, f)]

    def block(src_own, owner, sems, slot, where, h):
        xs = x_in.at[h] if src_own else x_all.at[owner, h]
        copies = [remote(xs, x_all.at[owner, h], sems.at[slot, h], xr.at[owner, h], where)]
        if h == 0:
            ws = w_in if src_own else w_all.at[owner]
            copies.append(remote(ws, w_all.at[owner], sems.at[slot, parts], wr.at[owner], where))
        return copies

    def shared(src_own, g, f, slot, where):
        src = s_in if src_own else s_at(g, f)
        return [remote(src, s_at(g, f), ss.at[slot], sr.at[g * n_fs + f], where)]

    def expert(src_own, f, t, slot):
        src = e_in.at[z * n_tp + tp] if src_own else e_at(gr, f, t)
        k = gr * plane + f * n_tp + t
        return [remote(src, e_at(gr, f, t), fs_sem.at[slot], er.at[k], dev(x_peer, z, tp))]

    own = tp * n_fs + z
    up, down = dev(gr, z + 1, tp), dev(gr, z - 1, tp)
    has_up, has_down = z < n_fs - 1, z > 0
    to_y, to_c, to_x = dev(gr, z, y_peer), dev(gr, z, c_peer), dev(x_peer, z, tp)
    pending = []

    def start(copies):
        for one in copies:
            one.start()

    def go(cond, copies):
        pending.append((cond, copies))
        if cond is None:
            start(copies)
        else:
            pl.when(cond)(lambda: start(copies))

    for h in range(parts):
        go(has_up, block(True, own, zs, 0, up, h))
        go(has_down, block(True, own, zs, 1, down, h))
        go(None, block(True, own, ys, 0, to_y, h))
        go(None, block(True, own, cs, 0, to_c, h))
    go(None, expert(True, z, tp, 0))
    go(has_up, shared(True, gr, z, 1, up))
    go(has_down, shared(True, gr, z, 2, down))
    go(None, shared(True, gr, z, 0, to_x))
    locals_ = [
        pltpu.make_async_copy(x_in, x_all.at[own], loc.at[0]),
        pltpu.make_async_copy(w_in, w_all.at[own], loc.at[1]),
        pltpu.make_async_copy(e_in.at[z * n_tp + tp], e_at(gr, z, tp), loc.at[2]),
        pltpu.make_async_copy(s_in, s_at(gr, z), loc.at[3]),
    ]
    start(locals_)

    def send_experts(want):
        for dz, dt, f, t in peers:
            if dz == want:
                mine = gr * plane + z * n_tp + tp
                go(None, [remote(
                    e_in.at[f * n_tp + t], e_at(gr, z, tp),
                    as_.at[dz * n_tp + dt], er.at[mine], dev(gr, f, t),
                )])

    def wait_expert(g, f, t):
        k = g * plane + f * n_tp + t
        remote(e_in.at[0], e_at(g, f, t), as_.at[0], er.at[k], to_x).wait_recv()

    def wait_block(owner, h):
        for one in block(True, owner, cs, 0, to_c, h):
            one.wait_recv()

    def wait_shared(g, f):
        shared(True, g, f, 0, to_x)[0].wait_recv()

    def pass_experts(want):
        for dz, dt, _, _ in peers:
            if dz == want:
                f, t = (z + n_fs - dz) % n_fs, (tp + n_tp - dt) % n_tp
                wait_expert(gr, f, t)
                go(None, expert(False, f, t, dz * n_tp + dt))

    send_experts(0)
    send_experts(1)
    for d in range(1, n_fs):
        for h in range(parts):
            for way in (0, 1):
                f = z - d if way == 0 else z + d
                there = f >= 0 if way == 0 else f < n_fs
                more = has_up if way == 0 else has_down
                onward = up if way == 0 else down
                owner = tp * n_fs + f
                slot = 2 * d + way
                pl.when(there)(functools.partial(wait_block, owner, h))
                go(there & more, block(False, owner, zs, slot, onward, h))
                go(there, block(False, owner, ys, slot, to_y, h))
                go(there, block(False, owner, cs, slot, to_c, h))
                if h == parts - 1:
                    pl.when(there)(functools.partial(wait_shared, gr, f))
                    go(there & more, shared(False, gr, f, 2 * slot + 1, onward))
                    go(there, shared(False, gr, f, 2 * slot, to_x))
        if d + 1 < n_fs:
            send_experts(d + 1)
        pass_experts(d - 1)
    pass_experts(n_fs - 1)
    for k in range(n_fs):
        f = (z + k) % n_fs
        owner = y_peer * n_fs + f
        for h in range(parts):
            wait_block(owner, h)
            go(None, block(False, owner, cs, 2 * n_fs + k, to_c, h))
    for f in range(n_fs):
        for t in range(n_tp):
            wait_expert(x_peer, f, t)
        wait_shared(x_peer, f)
        for yy in range(n_tp // CORES):
            for h in range(parts):
                wait_block((yy * CORES + 1 - c) * n_fs + f, h)
    for one in locals_:
        one.wait()

    def turn(k, carry):
        here = pl.ds(pl.multiple_of(k * cols_d, 128), cols_d)
        gate_out[here, :] = e_all[0, :, here].T
        up_out[here, :] = e_all[1, :, here].T
        s_gu[here, :] = s_out[0:2, :, here].reshape(2 * hid, cols_d).T
        return carry

    lax.fori_loop(0, n_gr * n_fs, turn, 0)

    step = 2
    chunk = min(width, 512)
    me = z * n_tp + tp

    def compute(group):
        def rows_of(k, carry):
            first = group * n_fs + k * step
            xs = x_all[pl.ds(first, step)].reshape(step * rows, width)
            ws = jnp.concatenate(
                [
                    jnp.broadcast_to(w_all[first + i, pl.ds(me, 1), :], (rows, rows)).T[:, :1]
                    for i in range(step)
                ],
                axis=0,
            )
            gate = jnp.dot(xs, gate_out[...], preferred_element_type=jnp.float32)
            upv = jnp.dot(xs, up_out[...], preferred_element_type=jnp.float32)
            act = (jax.nn.silu(gate) * upv * ws).astype(jnp.bfloat16)
            sh[...] = jnp.zeros_like(sh)

            @pl.when(z // step == k)
            def _():
                both = jnp.dot(
                    x_all[group * n_fs + z].reshape(rows, width), s_gu[...],
                    preferred_element_type=jnp.float32,
                )
                val = jax.nn.silu(both[:, :hid]) * both[:, hid:]
                sh[pl.ds(pl.multiple_of((z % step) * rows, 128), rows), :] = val.astype(jnp.bfloat16)

            extra = sh[...]

            def cols(j, inner):
                at = pl.ds(pl.multiple_of(j * chunk, 128), chunk)
                res = jnp.dot(act, e_all[2, :, at], preferred_element_type=jnp.float32)
                res = res + jnp.dot(extra, s_out[2, :, at], preferred_element_type=jnp.float32)
                part[pl.ds(first, step), :, :, at] = res.astype(jnp.bfloat16).reshape(
                    step, parts, sub, chunk
                )
                return inner

            return lax.fori_loop(0, width // chunk, cols, carry)

        lax.fori_loop(0, n_fs // step, rows_of, 0)

    other_y, other_c = 1 - y, 1 - c
    g_y = y_peer
    g_own = tp

    def wide(v):
        return v.astype(jnp.float32)

    def c_copy(i):
        group = (other_y if i == 0 else y) * CORES + other_c
        return remote(part.at[pl.ds(group * n_fs, n_fs)], rc.at[i], ks.at[i], kr.at[i], to_c)

    spots = []
    for d in range(n_fs - 1, -1, -1):
        for way in (0, 1):
            if d == 0 and way == 1:
                continue
            t = z + d if way == 0 else z - d
            spots.append((d, way, t, (t < n_fs) if way == 0 else (t >= 0)))

    def y_copy(t, h):
        return remote(part.at[g_y * n_fs + t, h], ry.at[t, h], qs.at[t, h], qr.at[t, h], to_y)

    def u_copy(t, h):
        return remote(part.at[g_own * n_fs + t, h], ru.at[t, h], us.at[t, h], ur.at[t, h], up)

    def d_copy(t, h):
        return remote(part.at[g_own * n_fs + t, h], rd.at[t, h], ds_.at[t, h], dr.at[t, h], down)

    def phase(i, carry):
        gy = jnp.where(i == 0, other_y, y)

        def one(k, inner):
            compute(gy * CORES + jnp.where(k == 0, other_c, c))

            @pl.when(k == 0)
            def _():
                pl.when(i == 0)(lambda: c_copy(0).start())
                pl.when(i == 1)(lambda: c_copy(1).start())

            return inner

        lax.fori_loop(0, 2, one, 0)

        @pl.when(i == 0)
        def _():
            c_copy(0).wait_recv()
            for _d, _way, t, there in spots:

                @pl.when(there)
                def _(t=t):
                    for h in range(parts):
                        at = g_y * n_fs + t
                        part[at, h] = (wide(part[at, h]) + wide(rc[0, t, h])).astype(jnp.bfloat16)
                        y_copy(t, h).start()

        return carry

    lax.fori_loop(0, 2, phase, 0)
    c_copy(1).wait_recv()

    for d, way, t, there in spots:

        @pl.when(there)
        def _(d=d, way=way, t=t):
            at = g_own * n_fs + t
            for h in range(parts):
                y_copy(t, h).wait_recv()
                total = wide(part[at, h]) + wide(rc[1, t, h]) + wide(ry[t, h])
                if d == 0:
                    mixed_out[h] = total.astype(jnp.bfloat16)

                    @pl.when(has_down & has_up)
                    def _():
                        u_copy(t, h).wait_recv()
                        d_copy(t, h).wait_recv()
                        mixed_out[h] = (total + wide(ru[t, h]) + wide(rd[t, h])).astype(jnp.bfloat16)

                    @pl.when(has_down & jnp.logical_not(has_up))
                    def _():
                        u_copy(t, h).wait_recv()
                        mixed_out[h] = (total + wide(ru[t, h])).astype(jnp.bfloat16)

                    @pl.when(has_up & jnp.logical_not(has_down))
                    def _():
                        d_copy(t, h).wait_recv()
                        mixed_out[h] = (total + wide(rd[t, h])).astype(jnp.bfloat16)
                else:
                    copy, arrived, before = (
                        (u_copy, ru, has_down) if way == 0 else (d_copy, rd, has_up)
                    )
                    part[at, h] = total.astype(jnp.bfloat16)

                    @pl.when(before)
                    def _():
                        copy(t, h).wait_recv()
                        part[at, h] = (total + wide(arrived[t, h])).astype(jnp.bfloat16)

                    copy(t, h).start()

    down_out[...] = e_all[2]
    for cond, copies in pending:
        if cond is None:
            for one in copies:
                one.wait_send()
        else:

            @pl.when(cond)
            def _(copies=copies):
                for one in copies:
                    one.wait_send()
    c_copy(0).wait_send()
    c_copy(1).wait_send()
    for d, way, t, there in spots:

        @pl.when(there)
        def _(d=d, way=way, t=t):
            for h in range(parts):
                y_copy(t, h).wait_send()
                if d:
                    (u_copy if way == 0 else d_copy)(t, h).wait_send()


def small_body(
    n_gr, n_fs, n_tp,
    prompt, train_gate, train_up, train_down, train_shared_gate, train_shared_up,
    train_shared_down, norm_gain, expert_ids, route_weight,
):
    experts, rows_d, hid = train_gate.shape
    rows, width = prompt.shape
    plane, full, parts = n_fs * n_tp, n_gr * n_fs, 2
    sub = rows // parts
    bf16 = jnp.bfloat16
    e_in = jnp.stack(
        (
            train_gate.transpose(0, 2, 1) * norm_gain,
            train_up.transpose(0, 2, 1) * norm_gain,
            train_down,
        ),
        axis=1,
    ).astype(bf16)
    s_in = jnp.stack(
        (train_shared_gate.T * norm_gain, train_shared_up.T * norm_gain, train_shared_down)
    ).astype(bf16)
    widened = prompt.astype(jnp.float32)
    normed = (
        widened * lax.rsqrt(jnp.mean(widened * widened, axis=-1, keepdims=True) + eps_norm)
    ).astype(bf16)
    named = expert_ids.T[None, :, :] == jnp.arange(experts, dtype=jnp.int32)[:, None, None]
    weights = jnp.sum(jnp.where(named, route_weight.T[None, :, :], 0.0), axis=1)

    vmem = pl.BlockSpec(memory_space=pltpu.VMEM)
    dma = pltpu.SemaphoreType.DMA
    shape = jax.ShapeDtypeStruct
    serve_gate, serve_up, serve_down, s_all, mixed_out = pl.pallas_call(
        functools.partial(plane_kernel, n_gr, n_fs, n_tp, parts),
        out_shape=(
            shape((width, n_tp * hid), bf16),
            shape((width, n_tp * hid), bf16),
            shape((n_tp * hid, width), bf16),
            shape((3, hid, width), bf16),
            shape((parts, sub, width), bf16),
        ),
        in_specs=[vmem] * 4,
        out_specs=(vmem,) * 5,
        scratch_shapes=[
            pltpu.VMEM((plane, parts, sub, width), bf16),
            pltpu.VMEM((plane, experts, rows), jnp.float32),
            pltpu.VMEM((3, n_tp * hid, width), bf16),
            pltpu.VMEM((width, 2 * hid), bf16),
            pltpu.VMEM((plane, parts, sub, width), bf16),
            pltpu.VMEM((2, n_fs, parts, sub, width), bf16),
            pltpu.VMEM((n_fs, parts, sub, width), bf16),
            pltpu.VMEM((n_fs, parts, sub, width), bf16),
            pltpu.VMEM((n_fs, parts, sub, width), bf16),
            pltpu.VMEM((2 * rows, hid), bf16),
            dma((plane, parts)), dma((plane,)), dma((n_gr * plane,)), dma((full,)),
            dma((2 * n_fs, parts + 1)), dma((2 * n_fs, parts + 1)), dma((3 * n_fs, parts + 1)),
            dma((plane,)), dma((plane,)), dma((4 * n_fs,)), dma((4,)),
            dma((2,)), dma((2,)),
            dma((n_fs, parts)), dma((n_fs, parts)), dma((n_fs, parts)),
            dma((n_fs, parts)), dma((n_fs, parts)), dma((n_fs, parts)),
        ],
        compiler_params=pltpu.CompilerParams(
            collective_id=0, has_side_effects=True, vmem_limit_bytes=VMEM_LIMIT
        ),
    )(normed.reshape(parts, sub, width), weights, e_in, s_in)
    return (
        serve_gate[None], serve_up[None], serve_down[None],
        s_all[0].T, s_all[1].T, s_all[2], mixed_out.reshape(rows, width),
    )


def regroup(stacked, lowered):
    stacked = lax.all_to_all(
        lax.all_to_all(stacked, "fs", split_axis=0, concat_axis=2, tiled=True),
        "tp",
        split_axis=0,
        concat_axis=3,
        tiled=True,
    )
    lowered = lax.all_to_all(
        lax.all_to_all(lowered, "fs", split_axis=0, concat_axis=2, tiled=True),
        "tp",
        split_axis=0,
        concat_axis=1,
        tiled=True,
    )
    return (stacked, lowered)


def body(
    prompt,
    train_gate,
    train_up,
    train_down,
    train_shared_gate,
    train_shared_up,
    train_shared_down,
    norm_gain,
    expert_ids,
    route_weight,
):
    gain_col = norm_gain[:, None]
    stacked = jnp.stack((train_gate * gain_col[None], train_up * gain_col[None]), axis=1).astype(
        jnp.bfloat16
    )
    lowered = train_down.astype(jnp.bfloat16)
    stacked, lowered = regroup(stacked, lowered)
    stacked, lowered = (
        lax.all_gather(stacked, "gr", axis=2, tiled=True),
        lax.all_gather(lowered, "gr", axis=2, tiled=True),
    )
    serve_gate = stacked[:, 0]
    serve_up = stacked[:, 1]
    serve_shared_gate, serve_shared_up, serve_shared_down = (
        lax.all_gather(
            (train_shared_gate * gain_col).astype(jnp.bfloat16), ("gr", "fs"), axis=0, tiled=True
        ),
        lax.all_gather(
            (train_shared_up * gain_col).astype(jnp.bfloat16), ("gr", "fs"), axis=0, tiled=True
        ),
        lax.all_gather(train_shared_down.astype(jnp.bfloat16), ("gr", "fs"), axis=1, tiled=True),
    )
    widened = prompt.astype(jnp.float32)
    normed = (
        widened * lax.rsqrt(jnp.mean(widened * widened, axis=-1, keepdims=True) + eps_norm)
    ).astype(jnp.bfloat16)
    block_rows = lax.all_gather(normed, "tp", axis=0, tiled=True)
    gate_val = jnp.dot(block_rows, serve_shared_gate, preferred_element_type=jnp.float32)
    up_val = jnp.dot(block_rows, serve_shared_up, preferred_element_type=jnp.float32)
    shared_act = (jax.nn.silu(gate_val) * up_val).astype(jnp.bfloat16)
    shared_sum = lax.psum_scatter(
        jnp.dot(shared_act, serve_shared_down, preferred_element_type=jnp.float32).astype(
            jnp.bfloat16
        ),
        "tp",
        scatter_dimension=0,
        tiled=True,
    ).astype(jnp.float32)
    row_count = prompt.shape[0]
    top_count = expert_ids.shape[1]
    model_width = prompt.shape[1]
    expert_count = lax.axis_size("fs") * lax.axis_size("tp")
    capacity = row_count * top_count // expert_count + 1
    flat_ids = expert_ids.reshape(-1)
    onehot = (flat_ids[:, None] == jnp.arange(expert_count, dtype=jnp.int32)[None, :]).astype(
        jnp.int32
    )
    earlier = jnp.cumsum(onehot, axis=0) - onehot
    places = jnp.sum(earlier * onehot, axis=1)
    slot_ids = (flat_ids * capacity + places).reshape(row_count, top_count)
    slot_range = jnp.arange(expert_count * capacity, dtype=jnp.int32)
    dispatch = jnp.any(slot_range[:, None, None] == slot_ids[None, :, :], axis=-1).astype(
        jnp.bfloat16
    )
    outgoing = jnp.dot(dispatch, normed, preferred_element_type=jnp.float32).astype(jnp.bfloat16)
    outgoing = outgoing.reshape(expert_count, capacity, model_width)
    arrived = lax.all_to_all(outgoing, ("fs", "tp"), split_axis=0, concat_axis=0, tiled=True)
    source_count, slot_count, width_here = arrived.shape
    arrived_rows = arrived.reshape(source_count * slot_count, width_here)
    gate_val = jnp.dot(arrived_rows, serve_gate[0], preferred_element_type=jnp.float32)
    up_val = jnp.dot(arrived_rows, serve_up[0], preferred_element_type=jnp.float32)
    hidden = (jax.nn.silu(gate_val) * up_val).astype(jnp.bfloat16)
    result = jnp.dot(hidden, lowered[0], preferred_element_type=jnp.float32).astype(jnp.bfloat16)
    result = result.reshape(source_count, slot_count, width_here)
    returned = lax.all_to_all(result, ("fs", "tp"), split_axis=0, concat_axis=0, tiled=True)
    picked = returned.reshape(expert_count * capacity, model_width)[slot_ids]
    routed = jnp.sum(route_weight[:, :, None] * picked.astype(jnp.float32), axis=1)
    mixed_out = (routed + shared_sum).astype(jnp.bfloat16)
    return (
        serve_gate,
        serve_up,
        lowered,
        serve_shared_gate,
        serve_shared_up,
        serve_shared_down,
        mixed_out,
    )


def solution(mesh):
    placed = (
        P(("gr", "fs", "tp"), None),
        P(None, ("gr", "fs"), "tp"),
        P(None, ("gr", "fs"), "tp"),
        P(None, "tp", ("gr", "fs")),
        P(("gr", "fs"), "tp"),
        P(("gr", "fs"), "tp"),
        P("tp", ("gr", "fs")),
        P(("gr", "fs")),
        P(("gr", "fs", "tp"), None),
        P(("gr", "fs", "tp"), None),
    )
    n_gr, n_fs, n_tp = (mesh.shape[name] for name in ("gr", "fs", "tp"))

    def chosen(prompt, *rest):
        held = n_fs * n_tp * prompt.size * prompt.dtype.itemsize * 5 // 2
        if n_gr == 2 and n_tp == 2 * CORES and n_fs % 2 == 0 and held < VMEM_PLAN:
            return small_body(n_gr, n_fs, n_tp, prompt, *rest)
        return body(prompt, *rest)

    return jax.shard_map(
        chosen,
        mesh=mesh,
        in_specs=placed,
        out_specs=(
            P(("fs", "tp"), None, None),
            P(("fs", "tp"), None, None),
            P(("fs", "tp"), None, None),
            P(None, "tp"),
            P(None, "tp"),
            P("tp", None),
            P(("gr", "fs", "tp"), None),
        ),
        check_vma=False,
    )
```

```python
import functools

import jax
import jax.numpy as jnp
from jax import lax
from jax.experimental import pallas as pl
from jax.experimental.pallas import tpu as pltpu
from jax.sharding import PartitionSpec as P

eps_norm = 1e-06
MESH = pl.DeviceIdType.MESH
CORES = 2
VMEM_PLAN = 40 * 2**20
VMEM_LIMIT = 60 * 2**20


def plane_kernel(
    n_gr, n_fs, n_tp, parts,
    p_ref, gt_ref, ut_ref, dn_ref, sg_ref, su_ref, sd_ref, gain_ref, ids_ref, rw_ref,
    gate_hbm, up_hbm, down_hbm, sg_hbm, su_hbm, sd_hbm, mixed_out,
    x_in, w_in, e_in, s_in, gate_out, up_out, down_out, s_out,
    x_all, w_all, e_all, s_gu, part, rc, ry, ru, rd, sh,
    xr, wr, er, sr, zs, ys, cs, as_, fs_sem, ss, loc,
    ks, kr, qs, qr, us, ur, ds_, dr, res_sem,
):
    gr, z, tp = lax.axis_index("gr"), lax.axis_index("fs"), lax.axis_index("tp")
    y, c = tp // CORES, tp % CORES
    y_peer = (1 - y) * CORES + c
    c_peer = y * CORES + 1 - c
    x_peer = 1 - gr
    plane = n_fs * n_tp
    _, hid, cols_d = s_in.shape
    sub, width = x_in.shape[1], x_in.shape[2]
    rows = parts * sub

    def dev(g, f, t):
        return {"gr": g, "fs": f, "tp": t}

    peers = [
        (dz, dt, (z + dz) % n_fs, (tp + dt) % n_tp)
        for dz in range(n_fs)
        for dt in range(n_tp)
        if dz or dt
    ]
    barrier = pltpu.get_barrier_semaphore()
    for _, _, f, t in peers:
        pl.semaphore_signal(barrier, inc=1, device_id=dev(gr, f, t), device_id_type=MESH)
    pl.semaphore_signal(barrier, inc=1, device_id=dev(x_peer, z, tp), device_id_type=MESH)

    gain = gain_ref[...]

    def cast(i, carry):
        e_in[i, 0] = (gt_ref[i] * gain).astype(jnp.bfloat16)
        e_in[i, 1] = (ut_ref[i] * gain).astype(jnp.bfloat16)
        e_in[i, 2] = dn_ref[i].astype(jnp.bfloat16)
        return carry

    s_in[0] = (sg_ref[...] * gain).astype(jnp.bfloat16)
    s_in[1] = (su_ref[...] * gain).astype(jnp.bfloat16)
    s_in[2] = sd_ref[...].astype(jnp.bfloat16)
    for h in range(parts):
        v = p_ref[h * sub : (h + 1) * sub, :].astype(jnp.float32)
        mean = jnp.mean(v * v, axis=-1, keepdims=True)
        x_in[h] = (v * lax.rsqrt(mean + eps_norm)).astype(jnp.bfloat16)
    table = jnp.zeros(w_in.shape, jnp.float32)
    which = lax.broadcasted_iota(jnp.int32, w_in.shape, 0)
    for k in range(ids_ref.shape[0]):
        table = table + jnp.where(ids_ref[k : k + 1, :] == which, rw_ref[k : k + 1, :], 0.0)
    w_in[...] = table
    lax.fori_loop(0, plane, cast, 0)
    pl.semaphore_wait(barrier, plane)

    def remote(src, dst, send, recv, where):
        return pltpu.make_async_remote_copy(
            src_ref=src, dst_ref=dst, send_sem=send, recv_sem=recv,
            device_id=where, device_id_type=MESH,
        )

    def cols_of(g, f):
        return pl.ds(pl.multiple_of((g * n_fs + f) * cols_d, 128), cols_d)

    def e_at(g, f, t):
        return e_all.at[g * n_fs + f, t]

    def s_at(g, f):
        return s_out.at[:, :, cols_of(g, f)]

    def block(src_own, owner, sems, slot, where, h):
        xs = x_in.at[h] if src_own else x_all.at[owner, h]
        copies = [remote(xs, x_all.at[owner, h], sems.at[slot, h], xr.at[owner, h], where)]
        if h == 0:
            ws = w_in if src_own else w_all.at[owner]
            copies.append(remote(ws, w_all.at[owner], sems.at[slot, parts], wr.at[owner], where))
        return copies

    def shared(src_own, g, f, slot, where):
        src = s_in if src_own else s_at(g, f)
        return [remote(src, s_at(g, f), ss.at[slot], sr.at[g * n_fs + f], where)]

    def expert(src_own, f, t, slot):
        src = e_in.at[z * n_tp + tp] if src_own else e_at(gr, f, t)
        k = gr * plane + f * n_tp + t
        return [remote(src, e_at(gr, f, t), fs_sem.at[slot], er.at[k], dev(x_peer, z, tp))]

    own = tp * n_fs + z
    up, down = dev(gr, z + 1, tp), dev(gr, z - 1, tp)
    has_up, has_down = z < n_fs - 1, z > 0
    to_y, to_c, to_x = dev(gr, z, y_peer), dev(gr, z, c_peer), dev(x_peer, z, tp)
    pending = []

    def start(copies):
        for one in copies:
            one.start()

    def go(cond, copies):
        pending.append((cond, copies))
        if cond is None:
            start(copies)
        else:
            pl.when(cond)(lambda: start(copies))

    for h in range(parts):
        go(has_up, block(True, own, zs, 0, up, h))
        go(has_down, block(True, own, zs, 1, down, h))
        go(None, block(True, own, ys, 0, to_y, h))
        go(None, block(True, own, cs, 0, to_c, h))
    go(None, expert(True, z, tp, 0))
    go(has_up, shared(True, gr, z, 1, up))
    go(has_down, shared(True, gr, z, 2, down))
    go(None, shared(True, gr, z, 0, to_x))
    locals_ = [
        pltpu.make_async_copy(x_in, x_all.at[own], loc.at[0]),
        pltpu.make_async_copy(w_in, w_all.at[own], loc.at[1]),
        pltpu.make_async_copy(e_in.at[z * n_tp + tp], e_at(gr, z, tp), loc.at[2]),
        pltpu.make_async_copy(s_in, s_at(gr, z), loc.at[3]),
    ]
    start(locals_)

    def send_experts(want):
        for dz, dt, f, t in peers:
            if dz == want:
                mine = gr * plane + z * n_tp + tp
                go(None, [remote(
                    e_in.at[f * n_tp + t], e_at(gr, z, tp),
                    as_.at[dz * n_tp + dt], er.at[mine], dev(gr, f, t),
                )])

    def wait_expert(g, f, t):
        k = g * plane + f * n_tp + t
        remote(e_in.at[0], e_at(g, f, t), as_.at[0], er.at[k], to_x).wait_recv()

    def wait_block(owner, h):
        for one in block(True, owner, cs, 0, to_c, h):
            one.wait_recv()

    def wait_shared(g, f):
        shared(True, g, f, 0, to_x)[0].wait_recv()

    def pass_experts(want):
        for dz, dt, _, _ in peers:
            if dz == want:
                f, t = (z + n_fs - dz) % n_fs, (tp + n_tp - dt) % n_tp
                wait_expert(gr, f, t)
                go(None, expert(False, f, t, dz * n_tp + dt))

    send_experts(0)
    send_experts(1)
    for d in range(1, n_fs):
        for h in range(parts):
            for way in (0, 1):
                f = z - d if way == 0 else z + d
                there = f >= 0 if way == 0 else f < n_fs
                more = has_up if way == 0 else has_down
                onward = up if way == 0 else down
                owner = tp * n_fs + f
                slot = 2 * d + way
                pl.when(there)(functools.partial(wait_block, owner, h))
                go(there & more, block(False, owner, zs, slot, onward, h))
                go(there, block(False, owner, ys, slot, to_y, h))
                go(there, block(False, owner, cs, slot, to_c, h))
                if h == parts - 1:
                    pl.when(there)(functools.partial(wait_shared, gr, f))
                    go(there & more, shared(False, gr, f, 2 * slot + 1, onward))
                    go(there, shared(False, gr, f, 2 * slot, to_x))
        if d + 1 < n_fs:
            send_experts(d + 1)
        pass_experts(d - 1)
    pass_experts(n_fs - 1)
    for k in range(n_fs):
        f = (z + k) % n_fs
        owner = y_peer * n_fs + f
        for h in range(parts):
            wait_block(owner, h)
            go(None, block(False, owner, cs, 2 * n_fs + k, to_c, h))
    for f in range(n_fs):
        for t in range(n_tp):
            wait_expert(x_peer, f, t)
        wait_shared(x_peer, f)
        for yy in range(n_tp // CORES):
            for h in range(parts):
                wait_block((yy * CORES + 1 - c) * n_fs + f, h)
    for one in locals_:
        one.wait()

    def turn(k, carry):
        here = pl.ds(pl.multiple_of(k * cols_d, 128), cols_d)
        gate_out[here, :] = e_all[k, :, 0].reshape(n_tp * hid, cols_d).T
        up_out[here, :] = e_all[k, :, 1].reshape(n_tp * hid, cols_d).T
        down_out[:, here] = e_all[k, :, 2].reshape(n_tp * hid, cols_d)
        s_gu[here, :] = s_out[0:2, :, here].reshape(2 * hid, cols_d).T
        return carry

    lax.fori_loop(0, n_gr * n_fs, turn, 0)
    results = [
        pltpu.make_async_copy(src, dst, res_sem.at[i])
        for i, (src, dst) in enumerate((
            (gate_out, gate_hbm), (up_out, up_hbm), (down_out, down_hbm),
            (s_out.at[0], sg_hbm), (s_out.at[1], su_hbm), (s_out.at[2], sd_hbm),
        ))
    ]
    start(results)

    step = 2
    chunk = min(width, 512)
    me = z * n_tp + tp

    def compute(group):
        def rows_of(k, carry):
            first = group * n_fs + k * step
            xs = x_all[pl.ds(first, step)].reshape(step * rows, width)
            ws = jnp.concatenate(
                [
                    jnp.broadcast_to(w_all[first + i, pl.ds(me, 1), :], (rows, rows)).T[:, :1]
                    for i in range(step)
                ],
                axis=0,
            )
            gate = jnp.dot(xs, gate_out[...], preferred_element_type=jnp.float32)
            upv = jnp.dot(xs, up_out[...], preferred_element_type=jnp.float32)
            act = (jax.nn.silu(gate) * upv * ws).astype(jnp.bfloat16)
            sh[...] = jnp.zeros_like(sh)

            @pl.when(z // step == k)
            def _():
                both = jnp.dot(
                    x_all[group * n_fs + z].reshape(rows, width), s_gu[...],
                    preferred_element_type=jnp.float32,
                )
                val = jax.nn.silu(both[:, :hid]) * both[:, hid:]
                sh[pl.ds(pl.multiple_of((z % step) * rows, 128), rows), :] = val.astype(jnp.bfloat16)

            extra = sh[...]

            def cols(j, inner):
                at = pl.ds(pl.multiple_of(j * chunk, 128), chunk)
                res = jnp.dot(act, down_out[:, at], preferred_element_type=jnp.float32)
                res = res + jnp.dot(extra, s_out[2, :, at], preferred_element_type=jnp.float32)
                part[pl.ds(first, step), :, :, at] = res.astype(jnp.bfloat16).reshape(
                    step, parts, sub, chunk
                )
                return inner

            return lax.fori_loop(0, width // chunk, cols, carry)

        lax.fori_loop(0, n_fs // step, rows_of, 0)

    other_y, other_c = 1 - y, 1 - c
    g_y = y_peer
    g_own = tp

    def wide(v):
        return v.astype(jnp.float32)

    def c_copy(i):
        group = (other_y if i == 0 else y) * CORES + other_c
        return remote(part.at[pl.ds(group * n_fs, n_fs)], rc.at[i], ks.at[i], kr.at[i], to_c)

    spots = []
    for d in range(n_fs - 1, -1, -1):
        for way in (0, 1):
            if d == 0 and way == 1:
                continue
            t = z + d if way == 0 else z - d
            spots.append((d, way, t, (t < n_fs) if way == 0 else (t >= 0)))

    def y_copy(t, h):
        return remote(part.at[g_y * n_fs + t, h], ry.at[t, h], qs.at[t, h], qr.at[t, h], to_y)

    def u_copy(t, h):
        return remote(part.at[g_own * n_fs + t, h], ru.at[t, h], us.at[t, h], ur.at[t, h], up)

    def d_copy(t, h):
        return remote(part.at[g_own * n_fs + t, h], rd.at[t, h], ds_.at[t, h], dr.at[t, h], down)

    def phase(i, carry):
        gy = jnp.where(i == 0, other_y, y)

        def one(k, inner):
            compute(gy * CORES + jnp.where(k == 0, other_c, c))

            @pl.when(k == 0)
            def _():
                pl.when(i == 0)(lambda: c_copy(0).start())
                pl.when(i == 1)(lambda: c_copy(1).start())

            return inner

        lax.fori_loop(0, 2, one, 0)

        @pl.when(i == 0)
        def _():
            c_copy(0).wait_recv()
            for _d, _way, t, there in spots:

                @pl.when(there)
                def _(t=t):
                    for h in range(parts):
                        at = g_y * n_fs + t
                        part[at, h] = (wide(part[at, h]) + wide(rc[0, t, h])).astype(jnp.bfloat16)
                        y_copy(t, h).start()

        return carry

    lax.fori_loop(0, 2, phase, 0)
    c_copy(1).wait_recv()

    for d, way, t, there in spots:

        @pl.when(there)
        def _(d=d, way=way, t=t):
            at = g_own * n_fs + t
            for h in range(parts):
                y_copy(t, h).wait_recv()
                total = wide(part[at, h]) + wide(rc[1, t, h]) + wide(ry[t, h])
                if d == 0:
                    mixed_out[h] = total.astype(jnp.bfloat16)

                    @pl.when(has_down & has_up)
                    def _():
                        u_copy(t, h).wait_recv()
                        d_copy(t, h).wait_recv()
                        mixed_out[h] = (total + wide(ru[t, h]) + wide(rd[t, h])).astype(jnp.bfloat16)

                    @pl.when(has_down & jnp.logical_not(has_up))
                    def _():
                        u_copy(t, h).wait_recv()
                        mixed_out[h] = (total + wide(ru[t, h])).astype(jnp.bfloat16)

                    @pl.when(has_up & jnp.logical_not(has_down))
                    def _():
                        d_copy(t, h).wait_recv()
                        mixed_out[h] = (total + wide(rd[t, h])).astype(jnp.bfloat16)
                else:
                    copy, arrived, before = (
                        (u_copy, ru, has_down) if way == 0 else (d_copy, rd, has_up)
                    )
                    part[at, h] = total.astype(jnp.bfloat16)

                    @pl.when(before)
                    def _():
                        copy(t, h).wait_recv()
                        part[at, h] = (total + wide(arrived[t, h])).astype(jnp.bfloat16)

                    copy(t, h).start()

    for one in results:
        one.wait()
    for cond, copies in pending:
        if cond is None:
            for one in copies:
                one.wait_send()
        else:

            @pl.when(cond)
            def _(copies=copies):
                for one in copies:
                    one.wait_send()
    c_copy(0).wait_send()
    c_copy(1).wait_send()
    for d, way, t, there in spots:

        @pl.when(there)
        def _(d=d, way=way, t=t):
            for h in range(parts):
                y_copy(t, h).wait_send()
                if d:
                    (u_copy if way == 0 else d_copy)(t, h).wait_send()


def small_body(
    n_gr, n_fs, n_tp,
    prompt, train_gate, train_up, train_down, train_shared_gate, train_shared_up,
    train_shared_down, norm_gain, expert_ids, route_weight,
):
    experts, rows_d, hid = train_gate.shape
    rows, width = prompt.shape
    plane, full, parts = n_fs * n_tp, n_gr * n_fs, 2
    sub = rows // parts
    bf16 = jnp.bfloat16
    vmem = pl.BlockSpec(memory_space=pltpu.VMEM)
    dma = pltpu.SemaphoreType.DMA
    shape = jax.ShapeDtypeStruct
    serve_gate, serve_up, serve_down, s_gate, s_up, s_down, mixed_out = pl.pallas_call(
        functools.partial(plane_kernel, n_gr, n_fs, n_tp, parts),
        out_shape=(
            shape((width, n_tp * hid), bf16),
            shape((width, n_tp * hid), bf16),
            shape((n_tp * hid, width), bf16),
            shape((hid, width), bf16),
            shape((hid, width), bf16),
            shape((hid, width), bf16),
            shape((parts, sub, width), bf16),
        ),
        in_specs=[vmem] * 10,
        out_specs=(pl.BlockSpec(memory_space=pl.ANY),) * 6 + (vmem,),
        scratch_shapes=[
            pltpu.VMEM((parts, sub, width), bf16),
            pltpu.VMEM((experts, rows), jnp.float32),
            pltpu.VMEM((experts, 3, hid, rows_d), bf16),
            pltpu.VMEM((3, hid, rows_d), bf16),
            pltpu.VMEM((width, n_tp * hid), bf16),
            pltpu.VMEM((width, n_tp * hid), bf16),
            pltpu.VMEM((n_tp * hid, width), bf16),
            pltpu.VMEM((3, hid, width), bf16),
            pltpu.VMEM((plane, parts, sub, width), bf16),
            pltpu.VMEM((plane, experts, rows), jnp.float32),
            pltpu.VMEM((full, n_tp, 3, hid, width // full), bf16),
            pltpu.VMEM((width, 2 * hid), bf16),
            pltpu.VMEM((plane, parts, sub, width), bf16),
            pltpu.VMEM((2, n_fs, parts, sub, width), bf16),
            pltpu.VMEM((n_fs, parts, sub, width), bf16),
            pltpu.VMEM((n_fs, parts, sub, width), bf16),
            pltpu.VMEM((n_fs, parts, sub, width), bf16),
            pltpu.VMEM((2 * rows, hid), bf16),
            dma((plane, parts)), dma((plane,)), dma((n_gr * plane,)), dma((full,)),
            dma((2 * n_fs, parts + 1)), dma((2 * n_fs, parts + 1)), dma((3 * n_fs, parts + 1)),
            dma((plane,)), dma((plane,)), dma((4 * n_fs,)), dma((4,)),
            dma((2,)), dma((2,)),
            dma((n_fs, parts)), dma((n_fs, parts)), dma((n_fs, parts)),
            dma((n_fs, parts)), dma((n_fs, parts)), dma((n_fs, parts)), dma((6,)),
        ],
        compiler_params=pltpu.CompilerParams(
            collective_id=0, has_side_effects=True, vmem_limit_bytes=VMEM_LIMIT
        ),
    )(
        prompt, train_gate.transpose(0, 2, 1), train_up.transpose(0, 2, 1), train_down,
        train_shared_gate.T, train_shared_up.T, train_shared_down, norm_gain[None, :],
        expert_ids.T, route_weight.T,
    )
    return (
        serve_gate[None], serve_up[None], serve_down[None],
        s_gate.T, s_up.T, s_down, mixed_out.reshape(rows, width),
    )


def regroup(stacked, lowered):
    stacked = lax.all_to_all(
        lax.all_to_all(stacked, "fs", split_axis=0, concat_axis=2, tiled=True),
        "tp",
        split_axis=0,
        concat_axis=3,
        tiled=True,
    )
    lowered = lax.all_to_all(
        lax.all_to_all(lowered, "fs", split_axis=0, concat_axis=2, tiled=True),
        "tp",
        split_axis=0,
        concat_axis=1,
        tiled=True,
    )
    return (stacked, lowered)


def body(
    prompt,
    train_gate,
    train_up,
    train_down,
    train_shared_gate,
    train_shared_up,
    train_shared_down,
    norm_gain,
    expert_ids,
    route_weight,
):
    gain_col = norm_gain[:, None]
    stacked = jnp.stack((train_gate * gain_col[None], train_up * gain_col[None]), axis=1).astype(
        jnp.bfloat16
    )
    lowered = train_down.astype(jnp.bfloat16)
    stacked, lowered = regroup(stacked, lowered)
    stacked, lowered = (
        lax.all_gather(stacked, "gr", axis=2, tiled=True),
        lax.all_gather(lowered, "gr", axis=2, tiled=True),
    )
    serve_gate = stacked[:, 0]
    serve_up = stacked[:, 1]
    serve_shared_gate, serve_shared_up, serve_shared_down = (
        lax.all_gather(
            (train_shared_gate * gain_col).astype(jnp.bfloat16), ("gr", "fs"), axis=0, tiled=True
        ),
        lax.all_gather(
            (train_shared_up * gain_col).astype(jnp.bfloat16), ("gr", "fs"), axis=0, tiled=True
        ),
        lax.all_gather(train_shared_down.astype(jnp.bfloat16), ("gr", "fs"), axis=1, tiled=True),
    )
    widened = prompt.astype(jnp.float32)
    normed = (
        widened * lax.rsqrt(jnp.mean(widened * widened, axis=-1, keepdims=True) + eps_norm)
    ).astype(jnp.bfloat16)
    block_rows = lax.all_gather(normed, "tp", axis=0, tiled=True)
    gate_val = jnp.dot(block_rows, serve_shared_gate, preferred_element_type=jnp.float32)
    up_val = jnp.dot(block_rows, serve_shared_up, preferred_element_type=jnp.float32)
    shared_act = (jax.nn.silu(gate_val) * up_val).astype(jnp.bfloat16)
    shared_sum = lax.psum_scatter(
        jnp.dot(shared_act, serve_shared_down, preferred_element_type=jnp.float32).astype(
            jnp.bfloat16
        ),
        "tp",
        scatter_dimension=0,
        tiled=True,
    ).astype(jnp.float32)
    row_count = prompt.shape[0]
    top_count = expert_ids.shape[1]
    model_width = prompt.shape[1]
    expert_count = lax.axis_size("fs") * lax.axis_size("tp")
    capacity = row_count * top_count // expert_count + 1
    flat_ids = expert_ids.reshape(-1)
    onehot = (flat_ids[:, None] == jnp.arange(expert_count, dtype=jnp.int32)[None, :]).astype(
        jnp.int32
    )
    earlier = jnp.cumsum(onehot, axis=0) - onehot
    places = jnp.sum(earlier * onehot, axis=1)
    slot_ids = (flat_ids * capacity + places).reshape(row_count, top_count)
    slot_range = jnp.arange(expert_count * capacity, dtype=jnp.int32)
    dispatch = jnp.any(slot_range[:, None, None] == slot_ids[None, :, :], axis=-1).astype(
        jnp.bfloat16
    )
    outgoing = jnp.dot(dispatch, normed, preferred_element_type=jnp.float32).astype(jnp.bfloat16)
    outgoing = outgoing.reshape(expert_count, capacity, model_width)
    arrived = lax.all_to_all(outgoing, ("fs", "tp"), split_axis=0, concat_axis=0, tiled=True)
    source_count, slot_count, width_here = arrived.shape
    arrived_rows = arrived.reshape(source_count * slot_count, width_here)
    gate_val = jnp.dot(arrived_rows, serve_gate[0], preferred_element_type=jnp.float32)
    up_val = jnp.dot(arrived_rows, serve_up[0], preferred_element_type=jnp.float32)
    hidden = (jax.nn.silu(gate_val) * up_val).astype(jnp.bfloat16)
    result = jnp.dot(hidden, lowered[0], preferred_element_type=jnp.float32).astype(jnp.bfloat16)
    result = result.reshape(source_count, slot_count, width_here)
    returned = lax.all_to_all(result, ("fs", "tp"), split_axis=0, concat_axis=0, tiled=True)
    picked = returned.reshape(expert_count * capacity, model_width)[slot_ids]
    routed = jnp.sum(route_weight[:, :, None] * picked.astype(jnp.float32), axis=1)
    mixed_out = (routed + shared_sum).astype(jnp.bfloat16)
    return (
        serve_gate,
        serve_up,
        lowered,
        serve_shared_gate,
        serve_shared_up,
        serve_shared_down,
        mixed_out,
    )


def solution(mesh):
    placed = (
        P(("gr", "fs", "tp"), None),
        P(None, ("gr", "fs"), "tp"),
        P(None, ("gr", "fs"), "tp"),
        P(None, "tp", ("gr", "fs")),
        P(("gr", "fs"), "tp"),
        P(("gr", "fs"), "tp"),
        P("tp", ("gr", "fs")),
        P(("gr", "fs")),
        P(("gr", "fs", "tp"), None),
        P(("gr", "fs", "tp"), None),
    )
    n_gr, n_fs, n_tp = (mesh.shape[name] for name in ("gr", "fs", "tp"))

    def chosen(prompt, *rest):
        held = n_fs * n_tp * prompt.size * prompt.dtype.itemsize * 5 // 2
        if n_gr == 2 and n_tp == 2 * CORES and n_fs % 2 == 0 and held < VMEM_PLAN:
            return small_body(n_gr, n_fs, n_tp, prompt, *rest)
        return body(prompt, *rest)

    return jax.shard_map(
        chosen,
        mesh=mesh,
        in_specs=placed,
        out_specs=(
            P(("fs", "tp"), None, None),
            P(("fs", "tp"), None, None),
            P(("fs", "tp"), None, None),
            P(None, "tp"),
            P(None, "tp"),
            P("tp", None),
            P(("gr", "fs", "tp"), None),
        ),
        check_vma=False,
    )
```
